32 devices in a mesh: sp: 8 (over z, core), tp: 4 (over y, x).
Axes of the slice: x: 2, y: 2, z: 4, core: 2. Of those that a mesh axis runs over, the one named last changes fastest.
Arguments:
- residual: bfloat16 [1024, 4096], P('sp', 'tp'), may hold values from -46 to 46
- query_small: bfloat16 [1024, 2048], P('sp', 'tp'), may hold values from -6 to 6
- key_narrow_group: bfloat16 [1024, 2048], P('sp', 'tp'), may hold values from -6 to 6
- query_large: bfloat16 [1024, 4096], P('sp', 'tp'), may hold values from -6 to 6
- key_large: bfloat16 [1024, 4096], P('sp', 'tp'), may hold values from -6 to 6
- values: bfloat16 [1024, 2, 2048], P('sp', None, 'tp'), may hold values from -6 to 6
- gates: bfloat16 [1024, 2, 2048], P('sp', None, 'tp'), may hold values from -6 to 6
- log_decay: float32 [1024, 2, 16], P('sp', None, 'tp'), may hold values from -0.65 to 0, as said below
- head_gain: float32 [2, 2048], P(None, 'tp'), may hold values from 0.1 to 1.9
- out_weight: bfloat16 [2, 2048, 4096], P(None, 'sp', 'tp'), may hold values from -0.09375 to 0.09375
- norm_gain: float32 [4096], P('tp'), may hold values from 0.1 to 1.9
- routes: int32 [1024, 2], P('sp'), may hold values from 0 to 7, all different within a row; in each aligned block of 128 rows (0 to 127, 128 to 255, ...) at most 64 rows name the same one
- route_weight: float32 [1024, 2], P('sp'), may hold values from 0.2 to 1
- expert_gate: bfloat16 [8, 4096, 2048], P('sp', None, 'tp'), may hold values from -0.09375 to 0.09375
- expert_up: bfloat16 [8, 4096, 2048], P('sp', None, 'tp'), may hold values from -0.09375 to 0.09375
- expert_down: bfloat16 [8, 2048, 4096], P('sp', None, 'tp'), may hold values from -0.5 to 0.5
Outputs:
- new_stream: bfloat16 [1024, 4096], P('sp', 'tp')
The draws below stay inside these ranges and needn't reach their ends.
Inputs may be any that keep to these rules, and one draw needn't show every extreme that they name: `routes`: each row names two different experts; in each aligned block of 128 rows no expert is named more than 64 times, a bound that some block reaches. `log_decay`: negative at every position.
All inputs are finite; a program needn't handle non-finite values.
Results may differ from the reference program's by a relative error of at most 0.019.
Values may be sent and summed in bfloat16 or wider, within the bound.
No kernel may reach another device: no remote copies, remote signals or barrier semaphores. Data moves between devices by JAX's collectives and lax.ppermute only.
A program may use at most 64 MiB of HBM per device.

```python
import math
import jax
import jax.numpy as jnp
import numpy as np
from jax import lax

D = 4096
H = 16
DKA = 128
DKB = 256
DV = 128
FF = 2048
TOK_DEV = 128
TOKENS = 1024
EXPERTS = 8
CAP = 64
N_SP = 8


def draw_residual(key, part):
    keys = jax.random.split(key, 3)
    base = jnp.clip(jax.random.normal(keys[0], (TOKENS, D), jnp.float32), -5.0, 5.0)
    ramp = jnp.arange(D, dtype=jnp.float32) / D
    coarse_estimate = jax.random.uniform(keys[1], (1, D), jnp.float32, 0.5, 1.5)
    columns = 0.3 * jnp.power(10.0, ramp)
    row_scale = jnp.exp(jax.random.uniform(keys[2], (TOKENS, 1), jnp.float32, -0.7, 0.7))
    return (base * columns[None, :] * coarse_estimate * row_scale).astype(jnp.bfloat16)


def draw_log_decay(key, part):
    keys = jax.random.split(key, 7)
    choose = jax.random.uniform(keys[0], (1, 2, H), jnp.float32)
    slow_heads = choose < 0.5
    fast_rate = jnp.exp(-jax.random.uniform(keys[1], (1, 2, H), jnp.float32, 3.4, 4.1))
    slow_rate = jax.random.uniform(keys[2], (1, 2, H), jnp.float32, 0.1, 0.4) / TOKENS
    decay_speed = jnp.where(slow_heads, slow_rate, fast_rate)
    block_count = TOKENS // TOK_DEV
    multiplier_term = jnp.exp(jax.random.uniform(keys[3], (block_count, 1, 1), jnp.float32, -0.69, 0.69))
    multiplier_term = jnp.repeat(multiplier_term, TOK_DEV, axis=0)
    coarse_estimate = jax.random.uniform(keys[4], (TOKENS, 2, H), jnp.float32, 0.5, 1.5)
    spots = jax.random.randint(keys[5], (3,), 0, TOKENS)
    hit_marker = jnp.any(jnp.arange(TOKENS)[:, None] == spots[None, :], axis=1)
    kept_fraction = jax.random.uniform(keys[6], (TOKENS, 1, 1), jnp.float32, 0.6, 0.8)
    spike_amount = jnp.where(hit_marker[:, None, None], jnp.log(kept_fraction), 0.0)
    return (-decay_speed * multiplier_term * coarse_estimate + spike_amount).astype(jnp.float32)


def levels(stream_key, shape, cuts, smallest, high):
    def one(dim, parts):
        draws = jax.random.uniform(jax.random.fold_in(jax.random.fold_in(stream_key, 6), dim), (parts,), jnp.float32, smallest / len(cuts), high / len(cuts))
        return jnp.repeat(jnp.exp(draws), shape[dim] // parts).reshape((-1,) + (1,) * (len(shape) - dim - 1))

    level = one(*cuts[0])
    for cut in cuts[1:]:
        level = level * one(*cut)
    return level


def shared_out(rng, own, number, rows, count, top, reach, slope):
    order = jax.random.permutation(rng, count)
    packed, usual = portions_of(count, rows * top, reach, slope, True), portions_of(count, rows * top, reach, slope, False)
    places = jnp.arange(count)

    def named(lengths, rotation):
        used = int((lengths > 0).sum())
        fixed = max(1, used // 4)
        moved = fixed + (places - fixed + rotation * (used - fixed)) % max(1, count - fixed)
        return jnp.zeros((count,), jnp.int32).at[order[jnp.where(places < fixed, places, moved)]].set(jnp.asarray(lengths, jnp.int32))

    lengths = jnp.where(number % 4 == 0, named(packed, number // 4), named(usual, number - number // 4 - 1))
    mixed = jax.random.permutation(jax.random.fold_in(own, 3), count)
    donor, sink = mixed[0:count // 2 * 2:2], mixed[1:count // 2 * 2:2]
    margin = jnp.minimum(lengths[donor] - 1, reach - lengths[sink]) // 2
    margin = jnp.where((donor == order[0]) | (sink == order[0]) | (lengths[sink] == 0), 0, jnp.maximum(margin, 0))
    moved = jax.random.randint(jax.random.fold_in(own, 4), (count // 2,), 0, 1 << 20) % (margin + 1)
    lengths = lengths.at[donor].add(-moved).at[sink].add(moved)
    items = jnp.searchsorted(jnp.cumsum(lengths), jnp.arange(rows * top), side="right").astype(jnp.int32)
    listing = items.reshape(top, rows).T
    listing = listing[jax.random.permutation(jax.random.fold_in(own, 1), rows)]
    rotation = jax.random.randint(jax.random.fold_in(own, 2), (rows, 1), 0, top)
    return jnp.take_along_axis(listing, (jnp.arange(top)[None, :] + rotation) % top, axis=1)


def portions_of(amount, total, reach, skew, full):
    weights = [(1 << 20) // math.isqrt(grade ** skew) + 1 for grade in range(1, amount + 1)]
    largest = reach if full else min(reach, max(-(-total // amount), total * weights[0] // sum(weights)))
    least = 1 if total - largest >= amount - 1 else 0
    given, spare = [largest] + [least] * (amount - 1), total - largest - least * (amount - 1)
    while spare > 0:
        candidates = [i for i in range(1, amount) if given[i] < largest] or [i for i in range(1, amount) if given[i] < reach]
        whole, left = sum([weights[i] for i in candidates]), spare
        for i in candidates:
            extra = min(reach - given[i], max(1, left * weights[i] // whole), spare)
            given[i] = given[i] + extra
            spare = spare - extra
    return np.array(given)


def scatter_about(own_key, dims, scale, most, cuts=(), held_as=jnp.bfloat16):
    result = jax.random.normal(own_key, dims, jnp.float32) * scale
    if len(cuts) > 0:
        result = levels(own_key, dims, cuts, -0.22, 0.18) * result
    return jnp.clip(result, min=-most, max=most).astype(held_as)


def setup_inputs(seed: int = 0) -> dict:
    key_of = jax.random.split(jax.random.key(seed), 17)
    residual = draw_residual(jax.random.fold_in(key_of[16], 71), 0)
    query_small = scatter_about(key_of[1], (TOKENS, H * DKA), 1.0, 6.0, ((0, 8), (1, 4)))
    key_narrow_group = scatter_about(key_of[2], (TOKENS, H * DKA), 1.0, 6.0, ((0, 8), (1, 4)))
    query_large = scatter_about(key_of[3], (TOKENS, H * DKB), 1.0, 6.0, ((0, 8), (1, 4)))
    key_large = scatter_about(key_of[4], (TOKENS, H * DKB), 1.0, 6.0, ((0, 8), (1, 4)))
    values = scatter_about(key_of[5], (TOKENS, 2, H * DV), 1.0, 6.0, ((0, 8), (2, 4)))
    gates = scatter_about(key_of[6], (TOKENS, 2, H * DV), 1.0, 6.0, ((0, 8), (2, 4)))
    log_decay = draw_log_decay(jax.random.fold_in(key_of[16], 71), 0)
    head_gain = jnp.clip(1.0 + 0.18 * jax.random.normal(key_of[8], (2, H * DV), jnp.float32), 0.1, 1.9)
    out_weight = scatter_about(key_of[9], (2, H * DV, D), (2 * H * DV) ** -0.5, 0.09375, ((1, 8), (2, 4)))
    norm_gain = jnp.clip(1.0 + 0.18 * jax.random.normal(key_of[10], (D,), jnp.float32), 0.1, 1.9)
    routes_keys = jax.random.split(jax.random.fold_in(key_of[11], 1), TOKENS // TOK_DEV)
    routes_turns = jax.random.permutation(jax.random.fold_in(key_of[11], 3), TOKENS // TOK_DEV)
    routes = jax.vmap(lambda own, number: shared_out(jax.random.fold_in(key_of[11], 2), own, number, TOK_DEV, EXPERTS, 2, CAP, 2))(routes_keys, routes_turns).reshape((TOKENS, 2))
    route_weight = jnp.clip(0.2 + 0.8 * jax.random.uniform(key_of[12], (TOKENS, 2), jnp.float32) ** levels(key_of[12], (TOKENS, 2), ((0, 8),), -0.2, 0.2), 0.2, 1.0)
    expert_gate = scatter_about(key_of[13], (EXPERTS, D, FF), D ** -0.5, 0.09375, ((0, 8), (2, 4)))
    expert_up = scatter_about(key_of[14], (EXPERTS, D, FF), D ** -0.5, 0.09375, ((0, 8), (2, 4)))
    expert_down = scatter_about(key_of[15], (EXPERTS, FF, D), (FF // 16) ** -0.5, 0.5, ((0, 8), (2, 4)))
    return {"residual": residual, "query_small": query_small, "key_narrow_group": key_narrow_group, "query_large": query_large, "key_large": key_large, "values": values, "gates": gates, "log_decay": log_decay, "head_gain": head_gain, "out_weight": out_weight, "norm_gain": norm_gain, "routes": routes, "route_weight": route_weight, "expert_gate": expert_gate, "expert_up": expert_up, "expert_down": expert_down}


EPS = 1e-06
THETA = 10000.0

def rotate(block, positions):
    half_dim = block.shape[-1] // 2
    inverse = jnp.power(THETA, -jnp.arange(half_dim, dtype=jnp.float32) * 2.0 / block.shape[-1])
    angles = positions[:, None, None] * inverse
    cosine_val, sine_val = (jnp.cos(angles), jnp.sin(angles))
    lower_half, upper_half = (block[..., :half_dim], block[..., half_dim:])
    return jnp.concatenate([lower_half * cosine_val - upper_half * sine_val, upper_half * cosine_val + lower_half * sine_val], axis=-1)

def block_terms(rot_queries, rot_keys, value_heads, rates):
    count = rates.shape[0]
    decay_sum = jnp.cumsum(rates, axis=0)
    by_head = decay_sum.T
    causal = (jnp.arange(count)[:, None] >= jnp.arange(count)[None, :])[None]
    spread = by_head[:, :, None] - by_head[:, None, :]
    weight = jnp.where(causal, jnp.exp(jnp.where(causal, spread, 0.0)), 0.0)
    scores = jnp.einsum('ihd,jhd->hij', rot_queries.astype(jnp.float32), rot_keys.astype(jnp.float32))
    weighted = (scores * weight).astype(jnp.bfloat16)
    within = jnp.einsum('hij,jhv->ihv', weighted.astype(jnp.float32), value_heads.astype(jnp.float32))
    block_end = decay_sum[-1]
    carried = (rot_keys.astype(jnp.float32) * jnp.exp(block_end[None, :] - decay_sum)[:, :, None]).astype(jnp.bfloat16)
    update = jnp.einsum('jhd,jhv->hdv', carried.astype(jnp.float32), value_heads.astype(jnp.float32))
    return (within, decay_sum, jnp.exp(block_end), update)

def final_result(rot_queries, decay_sum, within, state_in, gate_part, gain_part):
    cross_part = jnp.einsum('ihd,hdv->ihv', rot_queries.astype(jnp.float32), state_in, precision=lax.Precision.HIGHEST) * jnp.exp(decay_sum)[:, :, None]
    retained = within + cross_part
    scaled = retained * lax.rsqrt(lax.optimization_barrier(jnp.mean(retained * retained, axis=-1, keepdims=True)) + EPS)
    count, head_count, value_size = retained.shape
    gated = jax.nn.silu(gate_part.astype(jnp.float32)).reshape(count, head_count, value_size)
    return (scaled * gain_part.reshape(head_count, value_size) * gated).reshape(count, -1).astype(jnp.bfloat16)

def group_out(queries, keys_in, value_part, gate_part, rates, gain_part, key_size):
    length = queries.shape[0]
    head_count = rates.shape[1]
    value_size = value_part.shape[1] // head_count
    positions = jnp.arange(length, dtype=jnp.float32)
    rot_queries = rotate(queries.astype(jnp.float32).reshape(length, head_count, key_size), positions).astype(jnp.bfloat16)
    rot_keys = (rotate(keys_in.astype(jnp.float32).reshape(length, head_count, key_size), positions) * key_size ** (-0.5)).astype(jnp.bfloat16)
    value_heads = value_part.reshape(length, head_count, value_size)
    block_count = length // TOK_DEV

    def split_blocks(array):
        return array.reshape((block_count, TOK_DEV) + array.shape[1:])

    def advance(state, inputs):
        block_q, block_k, block_v, block_rates, block_gate = inputs
        within, decay_sum, fall, update = block_terms(block_q, block_k, block_v, block_rates)
        output = final_result(block_q, decay_sum, within, state, block_gate, gain_part)
        return (fall[:, None, None] * state + update, output)
    start_state = jnp.zeros((head_count, key_size, value_size), jnp.float32)
    _, outputs = lax.scan(advance, start_state, (split_blocks(rot_queries), split_blocks(rot_keys), split_blocks(value_heads), split_blocks(rates), split_blocks(gate_part)))
    return outputs.reshape(length, head_count * value_size)

def reference(residual, query_small, key_narrow_group, query_large, key_large, values, gates, log_decay, head_gain, out_weight, norm_gain, routes, route_weight, expert_gate, expert_up, expert_down):
    out_small = group_out(query_small, key_narrow_group, values[:, 0], gates[:, 0], log_decay[:, 0], head_gain[0], DKA)
    out_large = group_out(query_large, key_large, values[:, 1], gates[:, 1], log_decay[:, 1], head_gain[1], DKB)
    mixed = (jnp.dot(out_small, out_weight[0], preferred_element_type=jnp.float32) + jnp.dot(out_large, out_weight[1], preferred_element_type=jnp.float32)).astype(jnp.bfloat16)
    stream = residual.astype(jnp.float32) + mixed.astype(jnp.float32)
    normed = (stream * lax.rsqrt(lax.optimization_barrier(jnp.mean(stream * stream, axis=-1, keepdims=True)) + EPS) * norm_gain[None, :]).astype(jnp.bfloat16)
    experts = N_SP
    capacity = 4 * TOK_DEV // experts
    one_hot = (routes[:, :, None] == jnp.arange(experts, dtype=jnp.int32)[None, None, :]).astype(jnp.int32)
    one_hot = one_hot.reshape(N_SP, 2 * TOK_DEV, experts)
    before = jnp.cumsum(one_hot, axis=1) - one_hot
    slot_index = lax.optimization_barrier(jnp.sum(before * one_hot, axis=2)).reshape(TOKENS, 2)
    block_index = (jnp.arange(TOKENS, dtype=jnp.int32) // TOK_DEV).astype(jnp.int32)
    row_slot = (block_index[:, None] * capacity + slot_index).astype(jnp.int32)
    buffer = jnp.zeros((experts, N_SP * capacity, D), jnp.bfloat16)
    buffer = buffer.at[routes, row_slot].set(jnp.broadcast_to(normed[:, None, :], (TOKENS, 2, D)))

    def apply_expert(operands):
        rows_in, w_gate, w_up, w_down = operands
        gate_part = jnp.dot(rows_in, w_gate, preferred_element_type=jnp.float32)
        up_part = jnp.dot(rows_in, w_up, preferred_element_type=jnp.float32)
        hidden = (jax.nn.silu(gate_part) * up_part).astype(jnp.bfloat16)
        return jnp.dot(hidden, w_down, preferred_element_type=jnp.float32).astype(jnp.bfloat16)
    results = lax.map(apply_expert, (buffer, expert_gate, expert_up, expert_down))
    first_pick = results[routes[:, 0], row_slot[:, 0]].astype(jnp.float32)
    second_pick = results[routes[:, 1], row_slot[:, 1]].astype(jnp.float32)
    routed = route_weight[:, 0:1] * first_pick + route_weight[:, 1:2] * second_pick
    return (stream + routed).astype(jnp.bfloat16)
```

```python
import jax
import jax.numpy as jnp
from jax import lax
from jax.sharding import PartitionSpec as P

EPS = 1e-06
THETA = 10000.0
BF = jnp.bfloat16
F32 = jnp.float32


def rotate(block, positions):
    half_dim = block.shape[-1] // 2
    inverse = jnp.power(THETA, -jnp.arange(half_dim, dtype=F32) * 2.0 / block.shape[-1])
    angles = positions[:, None, None] * inverse
    cosine_val, sine_val = (jnp.cos(angles), jnp.sin(angles))
    lower_half, upper_half = (block[..., :half_dim], block[..., half_dim:])
    return jnp.concatenate(
        [
            lower_half * cosine_val - upper_half * sine_val,
            upper_half * cosine_val + lower_half * sine_val,
        ],
        axis=-1,
    )


def rotated(block, positions, head_count, scale=1.0):
    row_count = block.shape[0]
    heads = block.astype(F32).reshape(row_count, head_count, block.shape[1] // head_count)
    return (rotate(heads, positions) * scale).astype(BF)


def update_terms(rot_keys, value_heads, rates):
    decay_sum = jnp.cumsum(rates, axis=0)
    block_end = decay_sum[-1]
    carried = (
        rot_keys.astype(F32) * jnp.exp(block_end[None, :] - decay_sum)[:, :, None]
    ).astype(BF)
    update = jnp.einsum("jhd,jhv->hdv", carried, value_heads, preferred_element_type=F32)
    return decay_sum, block_end, update


def within_terms(rot_queries, rot_keys, value_heads, decay_sum):
    count = decay_sum.shape[0]
    by_head = decay_sum.T
    causal = (jnp.arange(count)[:, None] >= jnp.arange(count)[None, :])[None]
    spread = by_head[:, :, None] - by_head[:, None, :]
    weight = jnp.where(causal, jnp.exp(jnp.where(causal, spread, 0.0)), 0.0)
    scores = jnp.einsum("ihd,jhd->hij", rot_queries, rot_keys, preferred_element_type=F32)
    weighted = (scores * weight).astype(BF)
    return jnp.einsum("hij,jhv->ihv", weighted, value_heads, preferred_element_type=F32)


def final_result(rot_queries, decay_sum, within, state_in, gate_part, gain_part):
    cross_part = jnp.einsum(
        "ihd,hdv->ihv", rot_queries, state_in, preferred_element_type=F32
    ) * jnp.exp(decay_sum)[:, :, None]
    retained = within + cross_part
    scaled = retained * lax.rsqrt(jnp.mean(retained * retained, axis=-1, keepdims=True) + EPS)
    count, head_count, value_size = retained.shape
    gated = jax.nn.silu(gate_part.astype(F32)).reshape(count, head_count, value_size)
    return (
        (scaled * gain_part.reshape(head_count, value_size) * gated)
        .reshape(count, -1)
        .astype(BF)
    )


def per_device(
    residual,
    query_small,
    key_narrow_group,
    query_large,
    key_large,
    values,
    gates,
    log_decay,
    head_gain,
    out_weight,
    norm_gain,
    routes,
    route_weight,
    expert_gate,
    expert_up,
    expert_down,
):
    S, T = lax.axis_size("sp"), lax.axis_size("tp")
    Z = S // 2
    s, t = lax.axis_index("sp"), lax.axis_index("tp")
    z, c = s // 2, s % 2
    first = c == 0
    rows = residual.shape[0]
    piece = rows // T
    heads = log_decay.shape[2]
    width = residual.shape[1]

    def swap(x):
        return lax.ppermute(x, "sp", [(a, a ^ 1) for a in range(S)])

    def zshift(x, k, wrap=True):
        if k == 0:
            return x
        pairs = [(a, a + 2 * k) for a in range(S)]
        pairs = [(a, b % S) for a, b in pairs if wrap or 0 <= b < S]
        return lax.ppermute(x, "sp", pairs)

    def across(x, j):
        if j == 0:
            return x
        return lax.ppermute(x, "tp", [(a, a ^ j) for a in range(T)])

    def pick(x, i):
        return lax.dynamic_index_in_dim(x, i, 0, keepdims=False)

    def by_xor(x, axis):
        bit = 1
        while bit < T:
            shape = x.shape
            split = x.reshape(shape[:axis] + (T // (2 * bit), 2, bit) + shape[axis + 1 :])
            flipped = jnp.flip(split, axis + 1)
            x = jnp.where((t // bit) % 2 == 1, flipped, split).reshape(shape)
            bit *= 2
        return x

    def ordered(mine, other):
        return jnp.where(first, mine, other), jnp.where(first, other, mine)

    weight_own = [across(out_weight, j) for j in range(T)]
    weight_other = [swap(w) for w in weight_own]
    residual_pieces = residual.reshape(T, piece, width)
    residual_rows = [across(pick(residual_pieces, t ^ j), j) for j in range(T)]
    gain_parts = [across(norm_gain, j) for j in range(T)]

    experts = S
    capacity = 4 * rows // experts
    one_hot = (routes[:, :, None] == jnp.arange(experts, dtype=jnp.int32)).astype(jnp.int32)
    one_hot = one_hot.reshape(2 * rows, experts)
    before = jnp.cumsum(one_hot, axis=0) - one_hot
    slot_index = jnp.sum(before * one_hot, axis=1).reshape(rows, 2)
    info = jnp.concatenate(
        [routes.astype(F32), slot_index.astype(F32), route_weight, route_weight], axis=1
    )
    info_pair = jnp.stack([info, swap(info)])
    infos = [zshift(info_pair, k) for k in range(Z)]

    positions = (s * rows + jnp.arange(rows, dtype=jnp.int32)).astype(F32)
    value_a = values[:, 0].reshape(rows, heads, -1)
    value_b = values[:, 1].reshape(rows, heads, -1)
    size_a, size_b = query_small.shape[1] // heads, query_large.shape[1] // heads
    key_a = rotated(key_narrow_group, positions, heads, size_a ** (-0.5))
    key_b = rotated(key_large, positions, heads, size_b ** (-0.5))
    decay_a, end_a, update_a = update_terms(key_a, value_a, log_decay[:, 0])
    decay_b, end_b, update_b = update_terms(key_b, value_b, log_decay[:, 1])
    half_a, half_b = size_a // 2, size_b // 2

    def spread_rows(ends):
        return jnp.concatenate(
            [
                jnp.broadcast_to(ends[0][:, None, None], (heads, half_a, 1)),
                jnp.broadcast_to(ends[1][:, None, None], (heads, half_b, 1)),
            ],
            axis=1,
        )

    ends = jnp.stack([end_a, end_b])
    lower = jnp.concatenate([update_a[:, :half_a], update_b[:, :half_b]], axis=1)
    upper = jnp.concatenate([update_a[:, half_a:], update_b[:, half_b:]], axis=1)
    mine, theirs = ordered(lower, upper)
    got = swap(theirs)
    ends_got = swap(ends)
    update_0, update_1 = ordered(mine, got)
    ends_0, ends_1 = ordered(ends, ends_got)
    chip_update = (spread_rows(jnp.exp(ends_1)) * update_0 + update_1).astype(BF)
    chip_ends = ends_0 + ends_1
    arrived = [zshift(chip_update, k, False) for k in range(1, Z)]
    arrived_ends = [zshift(chip_ends, k, False) for k in range(1, Z)]
    state = arrived[0].astype(F32)
    passed = arrived_ends[0]
    for k in range(1, Z - 1):
        state = state + spread_rows(jnp.exp(passed)) * arrived[k].astype(F32)
        passed = passed + arrived_ends[k]
    state_0 = state.astype(BF)
    state_1 = (spread_rows(jnp.exp(ends_0)) * state + update_0).astype(BF)
    state_mine, state_theirs = ordered(state_0, state_1)
    state_got = swap(state_theirs)
    state_lower, state_upper = ordered(state_mine, state_got)
    state_a = jnp.concatenate([state_lower[:, :half_a], state_upper[:, :half_a]], axis=1)
    state_b = jnp.concatenate([state_lower[:, half_a:], state_upper[:, half_a:]], axis=1)

    query_a = rotated(query_small, positions, heads)
    query_b = rotated(query_large, positions, heads)
    within_a = within_terms(query_a, key_a, value_a, decay_a)
    within_b = within_terms(query_b, key_b, value_b, decay_b)
    output_a = final_result(query_a, decay_a, within_a, state_a, gates[:, 0], head_gain[0])
    output_b = final_result(query_b, decay_b, within_b, state_b, gates[:, 1], head_gain[1])

    stacked = jnp.stack([output_a, output_b], axis=1)
    pieces = stacked.reshape(T, piece, 2, stacked.shape[2])
    parts = jnp.stack([across(pick(pieces, t ^ j), j) for j in range(T)])
    depth = 2 * out_weight.shape[1]
    full = by_xor(parts, 0).transpose(1, 2, 0, 3)
    full = full.reshape(piece, 2, Z, depth).transpose(2, 0, 1, 3)
    sent = jnp.stack([zshift(pick(full, (z + k) % Z), k) for k in range(Z)])
    sent = sent.reshape(Z * piece, 2, 2, depth // 2).transpose(2, 0, 1, 3)
    sent = sent.reshape(2, Z * piece, depth)
    left_own, left_other = pick(sent, c), pick(sent, 1 - c)
    products = [
        jnp.dot(left_own, weight_own[j].reshape(depth, width), preferred_element_type=F32)
        + jnp.dot(left_other, weight_other[j].reshape(depth, width), preferred_element_type=F32)
        for j in range(T)
    ]
    product = jnp.stack([p.reshape(Z, piece, width) for p in products], axis=1)
    outgoing = product.astype(BF)
    mixed = product[0]
    for k in range(1, Z):
        mixed = mixed + zshift(outgoing[k], -k).astype(F32)
    mixed = mixed.astype(BF)
    stream_rows = jnp.stack(residual_rows).astype(F32) + mixed.astype(F32)
    square_mean = jnp.sum(stream_rows * stream_rows, axis=(0, 2)) / (T * width)
    scale = lax.rsqrt(square_mean + EPS)[None, :, None]
    normed = (stream_rows * scale * jnp.stack(gain_parts)[:, None, :]).astype(BF)
    normed = by_xor(normed, 0).transpose(1, 0, 2).reshape(piece, T * width)

    mixed_back = by_xor(jnp.stack([across(mixed[j], j) for j in range(T)]), 0)
    stream = residual.astype(F32) + mixed_back.reshape(rows, width).astype(F32)

    own = s.astype(F32)
    slots = jnp.arange(capacity, dtype=jnp.int32).astype(F32)

    def slot_of(part):
        return jnp.where(
            part[:, 0] == own, part[:, 2], jnp.where(part[:, 1] == own, part[:, 3], -1.0)
        )

    def choose(part):
        swapped = by_xor(part.reshape(T, piece, part.shape[1]), 0).reshape(part.shape)
        return (slots[:, None] == slot_of(swapped)[None, :]).astype(BF)

    def give(part, result):
        back = (slot_of(part)[:, None] == slots[None, :]).astype(BF)
        weight = jnp.where(
            part[:, 0] == own, part[:, 4], jnp.where(part[:, 1] == own, part[:, 5], 0.0)
        )
        return weight[:, None] * jnp.dot(back, result, preferred_element_type=F32)

    w_gate, w_up, w_down = (expert_gate[0], expert_up[0], expert_down[0])
    routed = None
    for k in range(Z):
        here = zshift(normed, k)
        block = jnp.concatenate([across(here, j) for j in range(T)], axis=0)
        block_other = swap(block)
        near, far = infos[k][0], infos[k][1]
        taken = jnp.concatenate(
            [
                jnp.dot(choose(near), block, preferred_element_type=F32),
                jnp.dot(choose(far), block_other, preferred_element_type=F32),
            ],
            axis=0,
        ).astype(BF)
        gate_part = jnp.dot(taken, w_gate, preferred_element_type=F32)
        up_part = jnp.dot(taken, w_up, preferred_element_type=F32)
        hidden = (jax.nn.silu(gate_part) * up_part).astype(BF)
        hidden = by_xor(jnp.stack([across(hidden, j) for j in range(T)]), 0)
        hidden = hidden.transpose(1, 0, 2).reshape(2 * capacity, -1)
        result = jnp.dot(hidden, w_down, preferred_element_type=F32).astype(BF)
        near_part = give(near, result[:capacity])
        far_part = give(far, result[capacity:]).astype(BF)
        summed = near_part + swap(far_part).astype(F32)
        if k > 0:
            summed = zshift(summed.astype(BF), -k).astype(F32)
        routed = summed if routed is None else routed + summed
    return (stream + routed).astype(BF)


def solution(mesh):
    placed = (
        P("sp", "tp"),
        P("sp", "tp"),
        P("sp", "tp"),
        P("sp", "tp"),
        P("sp", "tp"),
        P("sp", None, "tp"),
        P("sp", None, "tp"),
        P("sp", None, "tp"),
        P(None, "tp"),
        P(None, "sp", "tp"),
        P("tp"),
        P("sp", None),
        P("sp", None),
        P("sp", None, "tp"),
        P("sp", None, "tp"),
        P("sp", None, "tp"),
    )
    return jax.shard_map(
        per_device, mesh=mesh, in_specs=placed, out_specs=P("sp", "tp"), check_vma=False
    )
```

```python
import functools

import jax
import jax.numpy as jnp
import numpy as np
from jax import lax
from jax.experimental import pallas as pl
from jax.experimental.pallas import tpu as pltpu
from jax.sharding import PartitionSpec as P


EPS = 1e-06
THETA = 10000.0
BF = jnp.bfloat16
F32 = jnp.float32


END_ROWS = 8
SENT_ROWS = 16

VMEM = pl.BlockSpec(memory_space=pltpu.VMEM)


def inverses(size):
    powers = THETA ** (-np.arange(size // 2, dtype=np.float64) * 2.0 / size)
    return jnp.asarray(powers[None, :], F32)


def first_core():
    return lax.rem(lax.axis_index("sp"), 2) == 0


def reversed_bits(number, count):
    bits = count.bit_length() - 1
    return sum(((number >> i) & 1) << (bits - 1 - i) for i in range(bits))


def column_block(j, count):
    return lax.axis_index("tp") ^ jnp.where(first_core(), j, reversed_bits(j, count))


def turned(ref, head, size, cosine, sine):
    half = size // 2
    lower = ref[:, head * size : head * size + half].astype(F32)
    upper = ref[:, head * size + half : (head + 1) * size].astype(F32)
    return lower * cosine - upper * sine, upper * cosine + lower * sine


def triangle(count, lower):
    i = lax.broadcasted_iota(jnp.int32, (count, count), 0)
    j = lax.broadcasted_iota(jnp.int32, (count, count), 1)
    return i >= j if lower else i <= j


def contract(a, b, dims, precision=None):
    return lax.dot_general(
        a, b, (dims, ((), ())), preferred_element_type=F32, precision=precision
    )


def update_kernel(
    heads, key_a, key_b, value, inverse_a, inverse_b, rates,
    rot_a, rot_b, mine, theirs, decay, cos_a, sin_a, cos_b, sin_b,
):
    count = rates.shape[2]
    first = first_core()
    spot = lax.axis_index("sp") * count
    for inverse, cos, sin in ((inverse_a, cos_a, sin_a), (inverse_b, cos_b, sin_b)):
        spots = lax.broadcasted_iota(jnp.int32, cos.shape, 0) + spot
        angle = spots.astype(F32) * inverse[...]
        cos[...] = jnp.cos(angle)
        sin[...] = jnp.sin(angle)
    tri = triangle(count, True).astype(F32)
    sums = jnp.concatenate(
        [
            contract(tri, rates[group], ((1,), (1,)), lax.Precision.HIGHEST)
            for group in range(2)
        ],
        axis=1,
    )
    decay[...] = sums
    left = jnp.exp(sums[count - 1 : count, :] - sums)
    value_size = value.shape[1] // (2 * heads)
    row = 0
    for group, (key, rot, cos, sin) in enumerate(
        ((key_a, rot_a, cos_a, sin_a), (key_b, rot_b, cos_b, sin_b))
    ):
        size = key.shape[1] // heads
        half = size // 2
        for head in range(heads):
            column = group * heads + head
            values = value[:, column * value_size : (column + 1) * value_size]
            factor = left[:, column : column + 1]
            updates = []
            for part, turn in enumerate(turned(key, head, size, cos[...], sin[...])):
                keys = (turn * size ** (-0.5)).astype(BF)
                start = head * size + part * half
                rot[:, start : start + half] = keys
                carried = (keys.astype(F32) * factor).astype(BF)
                updates.append(contract(carried, values, ((0,), (0,))))
            mine[head, row : row + half, :] = jnp.where(first, updates[0], updates[1])
            theirs[head, row : row + half, :] = jnp.where(first, updates[1], updates[0])
        row += half
    lanes = mine.shape[2]
    which = lax.broadcasted_iota(jnp.int32, (END_ROWS, lanes), 0)
    for head in range(heads):
        pair = [
            jnp.broadcast_to(
                sums[count - 1 : count, column : column + 1], (END_ROWS, lanes)
            )
            for column in (head, heads + head)
        ]
        block = jnp.where(which == 0, pair[0], pair[1])
        mine[head, row : row + END_ROWS, :] = block
        theirs[head, row : row + END_ROWS, :] = block


def chip_kernel(half_a, mine, got, out):
    first = first_core()
    heads, height, lanes = mine.shape
    row = height - END_ROWS
    which = lax.broadcasted_iota(jnp.int32, (SENT_ROWS, lanes), 0)
    for head in range(heads):
        one, two = mine[head], got[head]
        before, after = jnp.where(first, one, two), jnp.where(first, two, one)
        begin = 0
        block = jnp.zeros((SENT_ROWS, lanes), F32)
        for group, end in enumerate((half_a, row)):
            last = after[row + group : row + group + 1, :]
            out[head, begin:end, :] = (
                jnp.exp(last) * before[begin:end, :] + after[begin:end, :]
            ).astype(BF)
            begin = end
            total = before[row + group : row + group + 1, :] + last
            for digit in range(3):
                part = total.astype(BF).astype(F32)
                total = total - part
                block = jnp.where(which == 3 * group + digit, part, block)
        out[head, row : row + SENT_ROWS, :] = block.astype(BF)


def state_kernel(half_a, count, *refs):
    arrived, (mine, got, out_mine, out_theirs) = refs[:count], refs[count:]
    first = first_core()
    heads, height, lanes = mine.shape
    row = height - END_ROWS
    for head in range(heads):
        begin = 0
        for group, end in enumerate((half_a, row)):
            span = slice(begin, end)
            state = arrived[0][head, span, :].astype(F32)
            passed = jnp.zeros((1, lanes), F32)
            for k in range(1, count):
                block = arrived[k - 1][head, row : row + SENT_ROWS, :].astype(F32)
                for digit in range(3):
                    at = 3 * group + digit
                    passed = passed + block[at : at + 1, :]
                state = state + jnp.exp(passed) * arrived[k][head, span, :].astype(F32)
            at = row + group
            update = jnp.where(first, mine[head, span, :], got[head, span, :])
            last = jnp.where(first, mine[head, at : at + 1, :], got[head, at : at + 1, :])
            later = jnp.exp(last) * state + update
            out_mine[head, span, :] = jnp.where(first, state, later).astype(BF)
            out_theirs[head, span, :] = jnp.where(first, later, state).astype(BF)
            begin = end


def norm_kernel(parts, others, *refs):
    own, refs = refs[0], refs[1:]
    moved, refs = refs[:others], refs[others:]
    residual, gain, refs = refs[:parts], refs[parts : 2 * parts], refs[2 * parts :]
    normed, mixed, stream = refs[0], refs[1:-1], refs[-1]
    width = own.shape[2]
    square = None
    for j in range(parts):
        total = own[j]
        for ref in moved:
            total = total + ref[j].astype(F32)
        rounded = total.astype(BF)
        mixed[j][...] = rounded
        row = residual[j][...].astype(F32) + rounded.astype(F32)
        stream[j] = row
        part = jnp.sum(row * row, axis=1, keepdims=True)
        square = part if square is None else square + part
    scale = lax.rsqrt(square / (parts * width) + EPS)
    for j in range(parts):
        begin = pl.multiple_of(column_block(j, parts) * width, width)
        normed[:, pl.ds(begin, width)] = (stream[j] * scale * gain[j][...]).astype(BF)


def within_kernel(
    heads, query_a, query_b, key_a, key_b, value, cos_a, sin_a, cos_b, sin_b,
    decay, rates, gates, gain, rot_a, rot_b, within, factor,
):
    count = decay.shape[0]
    lower = triangle(count, True)
    upper = triangle(count, False).astype(F32)
    value_size = value.shape[1] // (2 * heads)
    gate = gates[...].astype(F32)
    factor[...] = gain[...] * (gate / (1.0 + jnp.exp(-gate)))
    for group, (query, key, rot, cos, sin) in enumerate(
        ((query_a, key_a, rot_a, cos_a, sin_a), (query_b, key_b, rot_b, cos_b, sin_b))
    ):
        size = key.shape[1] // heads
        half = size // 2
        across = contract(rates[group], upper, ((1,), (0,)), lax.Precision.HIGHEST)
        for head in range(heads):
            column = group * heads + head
            start = head * size
            low, high = turned(query, head, size, cos[...], sin[...])
            rot[:, start : start + half] = low.astype(BF)
            rot[:, start + half : start + size] = high.astype(BF)
            scores = contract(
                rot[:, start : start + size], key[:, start : start + size], ((1,), (1,))
            )
            spread = decay[:, column : column + 1] - across[head : head + 1, :]
            weight = jnp.where(lower, jnp.exp(jnp.where(lower, spread, 0.0)), 0.0)
            place = slice(column * value_size, (column + 1) * value_size)
            within[:, place] = contract(
                (scores * weight).astype(BF), value[:, place], ((1,), (0,))
            )


def output_kernel(
    heads, query_a, query_b, within, decay, mine, got, factor, *outs
):
    held = outs[-1]
    first = first_core()
    value_size = within.shape[1] // (2 * heads)
    row = 0
    for group, query in enumerate((query_a, query_b)):
        size = query.shape[1] // heads
        half = size // 2
        for head in range(heads):
            column = group * heads + head
            one, two = mine[head, row : row + half, :], got[head, row : row + half, :]
            start = head * size
            cross = contract(
                query[:, start : start + half], jnp.where(first, one, two), ((1,), (0,))
            ) + contract(
                query[:, start + half : start + size], jnp.where(first, two, one), ((1,), (0,))
            )
            span = slice(column * value_size, (column + 1) * value_size)
            retained = within[:, span] + cross * jnp.exp(decay[:, column : column + 1])
            mean = jnp.mean(retained * retained, axis=1, keepdims=True)
            held[:, span] = retained * lax.rsqrt(mean + EPS) * factor[:, span]
        row += half
    for j, out in enumerate(outs[:-1]):
        piece = out.shape[0]
        begin = pl.multiple_of(column_block(j, len(outs) - 1) * piece, piece)
        out[...] = held[pl.ds(begin, piece), :].astype(BF)


def per_device(
    residual,
    query_small,
    key_narrow_group,
    query_large,
    key_large,
    values,
    gates,
    log_decay,
    head_gain,
    out_weight,
    norm_gain,
    routes,
    route_weight,
    expert_gate,
    expert_up,
    expert_down,
):
    S, T = lax.axis_size("sp"), lax.axis_size("tp")
    Z = S // 2
    s, t = lax.axis_index("sp"), lax.axis_index("tp")
    z, c = s // 2, s % 2
    first = c == 0
    rows = residual.shape[0]
    piece = rows // T
    heads = log_decay.shape[2]
    width = residual.shape[1]

    def swap(x):
        return lax.ppermute(x, "sp", [(a, a ^ 1) for a in range(S)])

    def zshift(x, k, wrap=True):
        if k == 0:
            return x
        pairs = [(a, a + 2 * k) for a in range(S)]
        pairs = [(a, b % S) for a, b in pairs if wrap or 0 <= b < S]
        return lax.ppermute(x, "sp", pairs)

    def across(x, j):
        if j == 0:
            return x
        pairs = []
        for a in range(S):
            far = j if a % 2 == 0 else reversed_bits(j, T)
            pairs += [(a * T + b, a * T + (b ^ far)) for b in range(T)]
        return lax.ppermute(x, ("sp", "tp"), pairs)

    bits = [1 << i for i in range(T.bit_length() - 1)]

    def crossed(x, i):
        pairs = []
        for a in range(S):
            bit = bits[i] if a % 2 == 0 else bits[len(bits) - 1 - i]
            pairs += [(a * T + b, a * T + (b ^ bit)) for b in range(T)]
        return lax.ppermute(x, ("sp", "tp"), pairs)

    def gathered(x):
        parts, number = [x], 0
        for i in range(len(bits)):
            new = []
            for part in parts:
                new.append(crossed(part, i))
                number += 1
            parts = parts + new
        return parts

    def pick(x, i):
        return lax.dynamic_index_in_dim(x, i, 0, keepdims=False)

    def by_xor(x, axis):
        for bit in bits:
            shape = x.shape
            split = x.reshape(shape[:axis] + (T // (2 * bit), 2, bit) + shape[axis + 1 :])
            flipped = jnp.flip(split, axis + 1)
            x = jnp.where((t // bit) % 2 == 1, flipped, split).reshape(shape)
        return x

    def by_core(x, axis, core_zero):
        shape = x.shape
        n = len(bits)
        split = x.reshape(shape[:axis] + (2,) * n + shape[axis + 1 :])
        order = list(range(split.ndim))
        order[axis : axis + n] = order[axis : axis + n][::-1]
        return jnp.where(core_zero, x, split.transpose(order).reshape(shape))

    def ordered(mine, other):
        return jnp.where(first, mine, other), jnp.where(first, other, mine)

    size_a, size_b = query_small.shape[1] // heads, query_large.shape[1] // heads
    value_rows = values.reshape(rows, -1)
    rates = log_decay.transpose(1, 2, 0)

    def after(values, *earlier):
        return lax.optimization_barrier((values, earlier))[0]

    half_a, half_b = size_a // 2, size_b // 2
    height, value_size = half_a + half_b, value_rows.shape[1] // (2 * heads)
    halves = (heads, height + END_ROWS, value_size)
    key_a, key_b, mine, theirs, decay, *tables = pl.pallas_call(
        functools.partial(update_kernel, heads),
        out_shape=(
            jax.ShapeDtypeStruct(key_narrow_group.shape, BF),
            jax.ShapeDtypeStruct(key_large.shape, BF),
            jax.ShapeDtypeStruct(halves, F32),
            jax.ShapeDtypeStruct(halves, F32),
            jax.ShapeDtypeStruct((rows, 2 * heads), F32),
            jax.ShapeDtypeStruct((rows, half_a), F32),
            jax.ShapeDtypeStruct((rows, half_a), F32),
            jax.ShapeDtypeStruct((rows, half_b), F32),
            jax.ShapeDtypeStruct((rows, half_b), F32),
        ),
        in_specs=[VMEM] * 6,
        out_specs=(VMEM,) * 9,
        name="update",
    )(key_narrow_group, key_large, value_rows, inverses(size_a), inverses(size_b), rates)

    got = swap(theirs)
    chip_update = pl.pallas_call(
        functools.partial(chip_kernel, half_a),
        out_shape=jax.ShapeDtypeStruct((heads, height + SENT_ROWS, value_size), BF),
        in_specs=[VMEM, VMEM],
        out_specs=VMEM,
        name="chip",
    )(mine, got)
    arrived = [zshift(chip_update, k, False) for k in range(1, Z)]

    turned_a, turned_b, within, factor = pl.pallas_call(
        functools.partial(within_kernel, heads),
        out_shape=(
            jax.ShapeDtypeStruct(query_small.shape, BF),
            jax.ShapeDtypeStruct(query_large.shape, BF),
            jax.ShapeDtypeStruct(value_rows.shape, F32),
            jax.ShapeDtypeStruct(value_rows.shape, F32),
        ),
        in_specs=[VMEM] * 13,
        out_specs=(VMEM,) * 4,
        name="within",
    )(
        query_small, query_large, key_a, key_b, value_rows, *tables, decay, rates,
        gates.reshape(rows, -1), head_gain.reshape(1, -1),
    )

    weight_own = gathered(after(out_weight, theirs))
    residual_in, gain_in = after((residual, norm_gain), chip_update, within)
    residual_pieces = residual_in.reshape(T, piece, width)
    residual_rows = [across(pick(residual_pieces, column_block(j, T)), j) for j in range(T)]
    gain_parts = [across(gain_in, j) for j in range(T)]

    experts = S
    capacity = 4 * rows // experts
    one_hot = (routes[:, :, None] == jnp.arange(experts, dtype=jnp.int32)).astype(jnp.int32)
    one_hot = one_hot.reshape(2 * rows, experts)
    before = jnp.cumsum(one_hot, axis=0) - one_hot
    slot_index = jnp.sum(before * one_hot, axis=1).reshape(rows, 2)
    info = jnp.concatenate(
        [routes.astype(F32), slot_index.astype(F32), route_weight, route_weight], axis=1
    )
    state_mine, state_theirs = pl.pallas_call(
        functools.partial(state_kernel, half_a, Z - 1),
        out_shape=(jax.ShapeDtypeStruct((heads, height, value_size), BF),) * 2,
        in_specs=[VMEM] * (Z + 1),
        out_specs=(VMEM, VMEM),
        name="state",
    )(*after(arrived, within), mine, got)
    state_got = swap(state_theirs)
    parts = pl.pallas_call(
        functools.partial(output_kernel, heads),
        out_shape=(jax.ShapeDtypeStruct((piece, value_rows.shape[1]), BF),) * T,
        in_specs=[VMEM] * 7,
        out_specs=(VMEM,) * T,
        scratch_shapes=[pltpu.VMEM(value_rows.shape, F32)],
        name="output",
    )(
        turned_a, turned_b, within, decay, state_mine, state_got, factor
    )

    depth = 2 * out_weight.shape[1]
    parts = [across(parts[j], j) for j in range(T)]
    weight_other = [swap(w) for w in after(weight_own, parts)]
    parts = by_core(jnp.stack(parts), 0, first)
    sent = [zshift(pick(parts, ((z + k) % Z) ^ t), k) for k in range(Z)]
    sent = jnp.concatenate(sent, axis=0)
    pairs = [
        ordered(sent[:, (i - 1) * (depth // 2) : i * (depth // 2)], sent[:, i * (depth // 2) : (i + 1) * (depth // 2)])
        for i in (1, 3)
    ]
    left_own = jnp.concatenate([pairs[0][0], pairs[1][0]], axis=1)
    left_other = jnp.concatenate([pairs[0][1], pairs[1][1]], axis=1)
    weight_other = [weight_other[reversed_bits(j, T)] for j in range(T)]
    products = [
        jnp.dot(left_own, weight_own[j].reshape(depth, width), preferred_element_type=F32)
        + jnp.dot(left_other, weight_other[j].reshape(depth, width), preferred_element_type=F32)
        for j in range(T)
    ]
    product = jnp.stack([p.reshape(Z, piece, width) for p in products], axis=1)
    outgoing = product.astype(BF)
    info = after(info, outgoing)
    info_pair = jnp.stack([info, swap(info)])
    infos = [zshift(info_pair, k) for k in range(Z)]
    moved = [zshift(outgoing[k], -k) for k in range(1, Z)]
    *normed, = pl.pallas_call(
        functools.partial(norm_kernel, T, Z - 1),
        out_shape=(jax.ShapeDtypeStruct((piece, T * width), BF),)
        + (jax.ShapeDtypeStruct((piece, width), BF),) * T,
        in_specs=[VMEM] * (Z + 2 * T),
        out_specs=(VMEM,) * (T + 1),
        scratch_shapes=[pltpu.VMEM((T, piece, width), F32)],
        name="norm",
    )(product[0], *moved, *residual_rows, *[g.reshape(1, -1) for g in gain_parts])
    normed, mixed = normed[0], normed[1:]

    own = s.astype(F32)
    slots = jnp.arange(capacity, dtype=jnp.int32).astype(F32)

    def slot_of(part):
        return jnp.where(
            part[..., 0] == own, part[..., 2], jnp.where(part[..., 1] == own, part[..., 3], -1.0)
        )

    def choose(part, core_zero, pieces_first):
        n = part.shape[0]
        part = by_xor(part.reshape(n, T, piece, part.shape[2]), 1)
        slot = slot_of(by_core(part, 1, core_zero))
        numbers = jnp.arange(n, dtype=jnp.int32)
        same = numbers[:, None] == numbers[None, :]
        hit = slots[None, :, None, None, None] == slot[None, None]
        hit = hit & same[:, None, :, None, None]
        if pieces_first:
            hit = hit.transpose(0, 1, 3, 2, 4)
        return hit.astype(BF).reshape(n * capacity, n * rows)

    def give(part, result):
        back = (slot_of(part)[:, :, None] == slots[None, None, :]).astype(BF)
        weight = jnp.where(
            part[..., 0] == own, part[..., 4], jnp.where(part[..., 1] == own, part[..., 5], 0.0)
        )
        picked = jnp.einsum("kts,ksd->ktd", back, result, preferred_element_type=F32)
        return weight[..., None] * picked

    w_gate, w_up, w_down = (expert_gate[0], expert_up[0], expert_down[0])
    even = [k for k in range(Z) if k % 2 == 0]
    odd = [k for k in range(Z) if k % 2 == 1]
    here = {k: zshift(normed, k) for k in even + odd}
    back = [across(mixed[j], j) for j in range(T)]
    mixed_back = by_xor(by_core(jnp.stack(back), 0, first), 0)
    stream = residual.astype(F32) + mixed_back.reshape(rows, width).astype(F32)

    def expert_rows(group, parts, pieces_first):
        block = jnp.concatenate(parts, axis=0)
        block_other = swap(block)
        near = jnp.stack([infos[k][0] for k in group])
        far = jnp.stack([infos[k][1] for k in group])
        choices = choose(near, first, pieces_first), choose(far, c == 1, pieces_first)
        taken = jnp.concatenate(
            [
                jnp.dot(choices[0], block, preferred_element_type=F32),
                jnp.dot(choices[1], block_other, preferred_element_type=F32),
            ],
            axis=0,
        ).astype(BF)
        gate_part = jnp.dot(taken, w_gate, preferred_element_type=F32)
        up_part = jnp.dot(taken, w_up, preferred_element_type=F32)
        return (jax.nn.silu(gate_part) * up_part).astype(BF), near, far

    def expert_sums(group, parts, near, far):
        n = len(group)
        hidden = by_xor(by_core(jnp.stack(parts), 0, first), 0)
        hidden = hidden.transpose(1, 0, 2).reshape(2 * n * capacity, -1)
        result = jnp.dot(hidden, w_down, preferred_element_type=F32).astype(BF)
        result = result.reshape(2, n, capacity, width)
        far_part = swap(give(far, result[1]).astype(BF)).astype(F32)
        return give(near, result[0]) + far_part

    parts_even = [p for k in even for p in gathered(here[k])]
    joined = jnp.concatenate([here[k] for k in odd], axis=0)
    parts_odd = gathered(joined)
    hidden_even, near_even, far_even = expert_rows(even, parts_even, False)
    hidden_odd, near_odd, far_odd = expert_rows(odd, after(parts_odd, hidden_even), True)
    gathered_even = gathered(hidden_even)
    sums_even = expert_sums(even, after(gathered_even, hidden_odd), near_even, far_even)
    gathered_odd = gathered(hidden_odd)
    sums_odd = expert_sums(odd, after(gathered_odd, sums_even), near_odd, far_odd)
    routed = sums_even[0]
    for sums, group in ((sums_even, even), (sums_odd, odd)):
        for i, k in enumerate(group):
            if k > 0:
                routed = routed + zshift(sums[i].astype(BF), -k).astype(F32)
    return (stream + routed).astype(BF)


def solution(mesh):
    placed = (
        P("sp", "tp"),
        P("sp", "tp"),
        P("sp", "tp"),
        P("sp", "tp"),
        P("sp", "tp"),
        P("sp", None, "tp"),
        P("sp", None, "tp"),
        P("sp", None, "tp"),
        P(None, "tp"),
        P(None, "sp", "tp"),
        P("tp"),
        P("sp", None),
        P("sp", None),
        P("sp", None, "tp"),
        P("sp", None, "tp"),
        P("sp", None, "tp"),
    )

    return jax.shard_map(
        per_device, mesh=mesh, in_specs=placed, out_specs=P("sp", "tp"), check_vma=False
    )
```

```python
import functools

import jax
import jax.numpy as jnp
import numpy as np
from jax import lax
from jax.experimental import pallas as pl
from jax.experimental.pallas import tpu as pltpu
from jax.sharding import PartitionSpec as P


EPS = 1e-06
THETA = 10000.0
BF = jnp.bfloat16
F32 = jnp.float32


END_ROWS = 8
SENT_ROWS = 16

VMEM = pl.BlockSpec(memory_space=pltpu.VMEM)


def inverses(size):
    powers = THETA ** (-np.arange(size // 2, dtype=np.float64) * 2.0 / size)
    return jnp.asarray(powers[None, :], F32)


def first_core():
    return lax.rem(lax.axis_index("sp"), 2) == 0


def reversed_bits(number, count):
    bits = count.bit_length() - 1
    return sum(((number >> i) & 1) << (bits - 1 - i) for i in range(bits))


def column_block(j, count):
    return lax.axis_index("tp") ^ jnp.where(first_core(), j, reversed_bits(j, count))


def turned(ref, head, size, cosine, sine):
    half = size // 2
    lower = ref[:, head * size : head * size + half].astype(F32)
    upper = ref[:, head * size + half : (head + 1) * size].astype(F32)
    return lower * cosine - upper * sine, upper * cosine + lower * sine


def triangle(count, lower):
    i = lax.broadcasted_iota(jnp.int32, (count, count), 0)
    j = lax.broadcasted_iota(jnp.int32, (count, count), 1)
    return i >= j if lower else i <= j


def contract(a, b, dims, precision=None):
    return lax.dot_general(
        a, b, (dims, ((), ())), preferred_element_type=F32, precision=precision
    )


def update_kernel(
    heads, key_a, key_b, value, inverse_a, inverse_b, rates,
    rot_a, rot_b, mine, theirs, decay, cos_a, sin_a, cos_b, sin_b,
):
    count = rates.shape[2]
    first = first_core()
    spot = lax.axis_index("sp") * count
    for inverse, cos, sin in ((inverse_a, cos_a, sin_a), (inverse_b, cos_b, sin_b)):
        spots = lax.broadcasted_iota(jnp.int32, cos.shape, 0) + spot
        angle = spots.astype(F32) * inverse[...]
        cos[...] = jnp.cos(angle)
        sin[...] = jnp.sin(angle)
    tri = triangle(count, True).astype(F32)
    sums = jnp.concatenate(
        [
            contract(tri, rates[group], ((1,), (1,)), lax.Precision.HIGHEST)
            for group in range(2)
        ],
        axis=1,
    )
    decay[...] = sums
    left = jnp.exp(sums[count - 1 : count, :] - sums)
    value_size = value.shape[1] // (2 * heads)
    row = 0
    for group, (key, rot, cos, sin) in enumerate(
        ((key_a, rot_a, cos_a, sin_a), (key_b, rot_b, cos_b, sin_b))
    ):
        size = key.shape[1] // heads
        half = size // 2
        for head in range(heads):
            column = group * heads + head
            values = value[:, column * value_size : (column + 1) * value_size]
            factor = left[:, column : column + 1]
            updates = []
            for part, turn in enumerate(turned(key, head, size, cos[...], sin[...])):
                keys = (turn * size ** (-0.5)).astype(BF)
                start = head * size + part * half
                rot[:, start : start + half] = keys
                carried = (keys.astype(F32) * factor).astype(BF)
                updates.append(contract(carried, values, ((0,), (0,))))
            mine[head, row : row + half, :] = jnp.where(first, updates[0], updates[1])
            theirs[head, row : row + half, :] = jnp.where(first, updates[1], updates[0])
        row += half
    lanes = mine.shape[2]
    which = lax.broadcasted_iota(jnp.int32, (END_ROWS, lanes), 0)
    for head in range(heads):
        pair = [
            jnp.broadcast_to(
                sums[count - 1 : count, column : column + 1], (END_ROWS, lanes)
            )
            for column in (head, heads + head)
        ]
        block = jnp.where(which == 0, pair[0], pair[1])
        mine[head, row : row + END_ROWS, :] = block
        theirs[head, row : row + END_ROWS, :] = block


def chip_kernel(half_a, mine, got, out):
    first = first_core()
    heads, height, lanes = mine.shape
    row = height - END_ROWS
    which = lax.broadcasted_iota(jnp.int32, (SENT_ROWS, lanes), 0)
    for head in range(heads):
        one, two = mine[head], got[head]
        before, after = jnp.where(first, one, two), jnp.where(first, two, one)
        begin = 0
        block = jnp.zeros((SENT_ROWS, lanes), F32)
        for group, end in enumerate((half_a, row)):
            last = after[row + group : row + group + 1, :]
            out[head, begin:end, :] = (
                jnp.exp(last) * before[begin:end, :] + after[begin:end, :]
            ).astype(BF)
            begin = end
            total = before[row + group : row + group + 1, :] + last
            for digit in range(3):
                part = total.astype(BF).astype(F32)
                total = total - part
                block = jnp.where(which == 3 * group + digit, part, block)
        out[head, row : row + SENT_ROWS, :] = block.astype(BF)


def state_kernel(half_a, count, *refs):
    arrived, (mine, got, out_mine, out_theirs) = refs[:count], refs[count:]
    first = first_core()
    heads, height, lanes = mine.shape
    row = height - END_ROWS
    for head in range(heads):
        begin = 0
        for group, end in enumerate((half_a, row)):
            span = slice(begin, end)
            state = arrived[0][head, span, :].astype(F32)
            passed = jnp.zeros((1, lanes), F32)
            for k in range(1, count):
                block = arrived[k - 1][head, row : row + SENT_ROWS, :].astype(F32)
                for digit in range(3):
                    at = 3 * group + digit
                    passed = passed + block[at : at + 1, :]
                state = state + jnp.exp(passed) * arrived[k][head, span, :].astype(F32)
            at = row + group
            update = jnp.where(first, mine[head, span, :], got[head, span, :])
            last = jnp.where(first, mine[head, at : at + 1, :], got[head, at : at + 1, :])
            later = jnp.exp(last) * state + update
            out_mine[head, span, :] = jnp.where(first, state, later).astype(BF)
            out_theirs[head, span, :] = jnp.where(first, later, state).astype(BF)
            begin = end


def norm_kernel(parts, others, *refs):
    own, refs = refs[0], refs[1:]
    moved, refs = refs[:others], refs[others:]
    residual, gain, refs = refs[:parts], refs[parts : 2 * parts], refs[2 * parts :]
    normed, mixed, stream = refs[0], refs[1:-1], refs[-1]
    width = own.shape[2]
    square = None
    for j in range(parts):
        total = own[j]
        for ref in moved:
            total = total + ref[j].astype(F32)
        rounded = total.astype(BF)
        mixed[j][...] = rounded
        row = residual[j][...].astype(F32) + rounded.astype(F32)
        stream[j] = row
        part = jnp.sum(row * row, axis=1, keepdims=True)
        square = part if square is None else square + part
    scale = lax.rsqrt(square / (parts * width) + EPS)
    for j in range(parts):
        begin = pl.multiple_of(column_block(j, parts) * width, width)
        normed[:, pl.ds(begin, width)] = (stream[j] * scale * gain[j][...]).astype(BF)


def within_kernel(
    heads, query_a, query_b, key_a, key_b, value, cos_a, sin_a, cos_b, sin_b,
    decay, rates, gates, gain, rot_a, rot_b, within, factor,
):
    count = decay.shape[0]
    lower = triangle(count, True)
    upper = triangle(count, False).astype(F32)
    value_size = value.shape[1] // (2 * heads)
    gate = gates[...].astype(F32)
    factor[...] = gain[...] * (gate / (1.0 + jnp.exp(-gate)))
    for group, (query, key, rot, cos, sin) in enumerate(
        ((query_a, key_a, rot_a, cos_a, sin_a), (query_b, key_b, rot_b, cos_b, sin_b))
    ):
        size = key.shape[1] // heads
        half = size // 2
        across = contract(rates[group], upper, ((1,), (0,)), lax.Precision.HIGHEST)
        for head in range(heads):
            column = group * heads + head
            start = head * size
            low, high = turned(query, head, size, cos[...], sin[...])
            rot[:, start : start + half] = low.astype(BF)
            rot[:, start + half : start + size] = high.astype(BF)
            scores = contract(
                rot[:, start : start + size], key[:, start : start + size], ((1,), (1,))
            )
            spread = decay[:, column : column + 1] - across[head : head + 1, :]
            weight = jnp.where(lower, jnp.exp(jnp.where(lower, spread, 0.0)), 0.0)
            place = slice(column * value_size, (column + 1) * value_size)
            within[:, place] = contract(
                (scores * weight).astype(BF), value[:, place], ((1,), (0,))
            )


def output_kernel(
    heads, query_a, query_b, within, decay, mine, got, factor, *outs
):
    held = outs[-1]
    first = first_core()
    value_size = within.shape[1] // (2 * heads)
    row = 0
    for group, query in enumerate((query_a, query_b)):
        size = query.shape[1] // heads
        half = size // 2
        for head in range(heads):
            column = group * heads + head
            one, two = mine[head, row : row + half, :], got[head, row : row + half, :]
            start = head * size
            cross = contract(
                query[:, start : start + half], jnp.where(first, one, two), ((1,), (0,))
            ) + contract(
                query[:, start + half : start + size], jnp.where(first, two, one), ((1,), (0,))
            )
            span = slice(column * value_size, (column + 1) * value_size)
            retained = within[:, span] + cross * jnp.exp(decay[:, column : column + 1])
            mean = jnp.mean(retained * retained, axis=1, keepdims=True)
            held[:, span] = retained * lax.rsqrt(mean + EPS) * factor[:, span]
        row += half
    for j, out in enumerate(outs[:-1]):
        piece = out.shape[0]
        begin = pl.multiple_of(column_block(j, len(outs) - 1) * piece, piece)
        out[...] = held[pl.ds(begin, piece), :].astype(BF)


def per_device(
    residual,
    query_small,
    key_narrow_group,
    query_large,
    key_large,
    values,
    gates,
    log_decay,
    head_gain,
    out_weight,
    norm_gain,
    routes,
    route_weight,
    expert_gate,
    expert_up,
    expert_down,
):
    S, T = lax.axis_size("sp"), lax.axis_size("tp")
    Z = S // 2
    s, t = lax.axis_index("sp"), lax.axis_index("tp")
    z, c = s // 2, s % 2
    first = c == 0
    rows = residual.shape[0]
    piece = rows // T
    heads = log_decay.shape[2]
    width = residual.shape[1]

    def swap(x):
        return lax.ppermute(x, "sp", [(a, a ^ 1) for a in range(S)])

    def zshift(x, k, wrap=True):
        if k == 0:
            return x
        pairs = [(a, a + 2 * k) for a in range(S)]
        pairs = [(a, b % S) for a, b in pairs if wrap or 0 <= b < S]
        return lax.ppermute(x, "sp", pairs)

    def across(x, j):
        if j == 0:
            return x
        pairs = []
        for a in range(S):
            far = j if a % 2 == 0 else reversed_bits(j, T)
            pairs += [(a * T + b, a * T + (b ^ far)) for b in range(T)]
        return lax.ppermute(x, ("sp", "tp"), pairs)

    bits = [1 << i for i in range(T.bit_length() - 1)]

    def crossed(x, i):
        pairs = []
        for a in range(S):
            bit = bits[i] if a % 2 == 0 else bits[len(bits) - 1 - i]
            pairs += [(a * T + b, a * T + (b ^ bit)) for b in range(T)]
        return lax.ppermute(x, ("sp", "tp"), pairs)

    def gathered(x):
        parts, number = [x], 0
        for i in range(len(bits)):
            new = []
            for part in parts:
                new.append(crossed(part, i))
                number += 1
            parts = parts + new
        return parts

    def pick(x, i):
        return lax.dynamic_index_in_dim(x, i, 0, keepdims=False)

    def by_xor(x, axis):
        for bit in bits:
            shape = x.shape
            split = x.reshape(shape[:axis] + (T // (2 * bit), 2, bit) + shape[axis + 1 :])
            flipped = jnp.flip(split, axis + 1)
            x = jnp.where((t // bit) % 2 == 1, flipped, split).reshape(shape)
        return x

    def by_core(x, axis, core_zero):
        shape = x.shape
        n = len(bits)
        split = x.reshape(shape[:axis] + (2,) * n + shape[axis + 1 :])
        order = list(range(split.ndim))
        order[axis : axis + n] = order[axis : axis + n][::-1]
        return jnp.where(core_zero, x, split.transpose(order).reshape(shape))

    def ordered(mine, other):
        return jnp.where(first, mine, other), jnp.where(first, other, mine)

    size_a, size_b = query_small.shape[1] // heads, query_large.shape[1] // heads
    value_rows = values.reshape(rows, -1)
    rates = log_decay.transpose(1, 2, 0)

    def after(values, *earlier):
        return lax.optimization_barrier((values, earlier))[0]

    half_a, half_b = size_a // 2, size_b // 2
    height, value_size = half_a + half_b, value_rows.shape[1] // (2 * heads)
    halves = (heads, height + END_ROWS, value_size)
    key_a, key_b, mine, theirs, decay, *tables = pl.pallas_call(
        functools.partial(update_kernel, heads),
        out_shape=(
            jax.ShapeDtypeStruct(key_narrow_group.shape, BF),
            jax.ShapeDtypeStruct(key_large.shape, BF),
            jax.ShapeDtypeStruct(halves, F32),
            jax.ShapeDtypeStruct(halves, F32),
            jax.ShapeDtypeStruct((rows, 2 * heads), F32),
            jax.ShapeDtypeStruct((rows, half_a), F32),
            jax.ShapeDtypeStruct((rows, half_a), F32),
            jax.ShapeDtypeStruct((rows, half_b), F32),
            jax.ShapeDtypeStruct((rows, half_b), F32),
        ),
        in_specs=[VMEM] * 6,
        out_specs=(VMEM,) * 9,
        name="update",
    )(key_narrow_group, key_large, value_rows, inverses(size_a), inverses(size_b), rates)

    got = swap(theirs)
    chip_update = pl.pallas_call(
        functools.partial(chip_kernel, half_a),
        out_shape=jax.ShapeDtypeStruct((heads, height + SENT_ROWS, value_size), BF),
        in_specs=[VMEM, VMEM],
        out_specs=VMEM,
        name="chip",
    )(mine, got)
    arrived = [zshift(chip_update, k, False) for k in range(1, Z)]

    turned_a, turned_b, within, factor = pl.pallas_call(
        functools.partial(within_kernel, heads),
        out_shape=(
            jax.ShapeDtypeStruct(query_small.shape, BF),
            jax.ShapeDtypeStruct(query_large.shape, BF),
            jax.ShapeDtypeStruct(value_rows.shape, F32),
            jax.ShapeDtypeStruct(value_rows.shape, F32),
        ),
        in_specs=[VMEM] * 13,
        out_specs=(VMEM,) * 4,
        name="within",
    )(
        query_small, query_large, key_a, key_b, value_rows, *tables, decay, rates,
        *[after(x, chip_update).reshape(-1, 2 * heads * value_size) for x in (gates, head_gain)],
    )

    weight_own = gathered(after(out_weight, theirs))
    residual_in, gain_in = after((residual, norm_gain), chip_update, within)
    residual_pieces = residual_in.reshape(T, piece, width)
    residual_rows = [across(pick(residual_pieces, column_block(j, T)), j) for j in range(T)]
    gain_parts = [across(gain_in, j) for j in range(T)]

    state_mine, state_theirs = pl.pallas_call(
        functools.partial(state_kernel, half_a, Z - 1),
        out_shape=(jax.ShapeDtypeStruct((heads, height, value_size), BF),) * 2,
        in_specs=[VMEM] * (Z + 1),
        out_specs=(VMEM, VMEM),
        name="state",
    )(*after(arrived, within), mine, got)
    state_got = swap(state_theirs)
    parts = pl.pallas_call(
        functools.partial(output_kernel, heads),
        out_shape=(jax.ShapeDtypeStruct((piece, value_rows.shape[1]), BF),) * T,
        in_specs=[VMEM] * 7,
        out_specs=(VMEM,) * T,
        scratch_shapes=[pltpu.VMEM(value_rows.shape, F32)],
        name="output",
    )(
        turned_a, turned_b, within, decay, state_mine, state_got, factor
    )

    depth = 2 * out_weight.shape[1]
    parts = [across(parts[j], j) for j in range(T)]
    weight_other = [swap(w) for w in after(weight_own, parts)]
    parts = by_core(jnp.stack(parts), 0, first)
    sent = [zshift(pick(parts, ((z + k) % Z) ^ t), k) for k in range(Z)]
    sent = jnp.concatenate(sent, axis=0)
    pairs = [
        ordered(sent[:, (i - 1) * (depth // 2) : i * (depth // 2)], sent[:, i * (depth // 2) : (i + 1) * (depth // 2)])
        for i in (1, 3)
    ]
    left_own = jnp.concatenate([pairs[0][0], pairs[1][0]], axis=1)
    left_other = jnp.concatenate([pairs[0][1], pairs[1][1]], axis=1)
    weight_other = [weight_other[reversed_bits(j, T)] for j in range(T)]
    products = [
        jnp.dot(left_own, weight_own[j].reshape(depth, width), preferred_element_type=F32)
        + jnp.dot(left_other, weight_other[j].reshape(depth, width), preferred_element_type=F32)
        for j in range(T)
    ]
    product = jnp.stack([p.reshape(Z, piece, width) for p in products], axis=1)
    outgoing = product.astype(BF)
    moved = [zshift(outgoing[k], -k) for k in range(1, Z)]
    experts = S
    capacity = 4 * rows // experts
    routes, route_weight = after((routes, route_weight), moved)
    one_hot = (routes[:, :, None] == jnp.arange(experts, dtype=jnp.int32)).astype(jnp.int32)
    one_hot = one_hot.reshape(2 * rows, experts)
    before = jnp.cumsum(one_hot, axis=0) - one_hot
    slot_index = jnp.sum(before * one_hot, axis=1).reshape(rows, 2)
    info = jnp.concatenate(
        [routes.astype(F32), slot_index.astype(F32), route_weight, route_weight], axis=1
    )
    info_pair = jnp.stack([info, swap(info)])
    infos = [zshift(info_pair, k) for k in range(Z)]
    *normed, = pl.pallas_call(
        functools.partial(norm_kernel, T, Z - 1),
        out_shape=(jax.ShapeDtypeStruct((piece, T * width), BF),)
        + (jax.ShapeDtypeStruct((piece, width), BF),) * T,
        in_specs=[VMEM] * (Z + 2 * T),
        out_specs=(VMEM,) * (T + 1),
        scratch_shapes=[pltpu.VMEM((T, piece, width), F32)],
        name="norm",
    )(product[0], *moved, *residual_rows, *[g.reshape(1, -1) for g in gain_parts])
    normed, mixed = normed[0], normed[1:]

    own = s.astype(F32)
    slots = jnp.arange(capacity, dtype=jnp.int32).astype(F32)

    def slot_of(part):
        return jnp.where(
            part[..., 0] == own, part[..., 2], jnp.where(part[..., 1] == own, part[..., 3], -1.0)
        )

    def choose(part, core_zero, pieces_first):
        n = part.shape[0]
        part = by_xor(part.reshape(n, T, piece, part.shape[2]), 1)
        slot = slot_of(by_core(part, 1, core_zero))
        numbers = jnp.arange(n, dtype=jnp.int32)
        same = numbers[:, None] == numbers[None, :]
        hit = slots[None, :, None, None, None] == slot[None, None]
        hit = hit & same[:, None, :, None, None]
        if pieces_first:
            hit = hit.transpose(0, 1, 3, 2, 4)
        return hit.astype(BF).reshape(n * capacity, n * rows)

    def give(part, result):
        back = (slot_of(part)[:, :, None] == slots[None, None, :]).astype(BF)
        weight = jnp.where(
            part[..., 0] == own, part[..., 4], jnp.where(part[..., 1] == own, part[..., 5], 0.0)
        )
        picked = jnp.einsum("kts,ksd->ktd", back, result, preferred_element_type=F32)
        return weight[..., None] * picked

    w_gate, w_up, w_down = (expert_gate[0], expert_up[0], expert_down[0])
    even = [k for k in range(Z) if k % 2 == 0]
    odd = [k for k in range(Z) if k % 2 == 1]
    here = {k: zshift(normed, k) for k in even + odd}
    back = [across(mixed[j], j) for j in range(T)]
    mixed_back = by_xor(by_core(jnp.stack(back), 0, first), 0)
    stream = residual.astype(F32) + mixed_back.reshape(rows, width).astype(F32)

    def expert_rows(group, parts, pieces_first):
        block = jnp.concatenate(parts, axis=0)
        block_other = swap(block)
        known = after([infos[k] for k in group], block)
        near = jnp.stack([info[0] for info in known])
        far = jnp.stack([info[1] for info in known])
        choices = choose(near, first, pieces_first), choose(far, c == 1, pieces_first)
        taken = jnp.concatenate(
            [
                jnp.dot(choices[0], block, preferred_element_type=F32),
                jnp.dot(choices[1], block_other, preferred_element_type=F32),
            ],
            axis=0,
        ).astype(BF)
        gate_part = jnp.dot(taken, w_gate, preferred_element_type=F32)
        up_part = jnp.dot(taken, w_up, preferred_element_type=F32)
        return (jax.nn.silu(gate_part) * up_part).astype(BF), near, far

    def expert_sums(group, parts, near, far):
        n = len(group)
        hidden = by_xor(by_core(jnp.stack(parts), 0, first), 0)
        hidden = hidden.transpose(1, 0, 2).reshape(2 * n * capacity, -1)
        result = jnp.dot(hidden, w_down, preferred_element_type=F32).astype(BF)
        result = result.reshape(2, n, capacity, width)
        far_part = swap(give(far, result[1]).astype(BF)).astype(F32)
        return give(near, result[0]) + far_part

    parts_even = [p for k in even for p in gathered(here[k])]
    joined = jnp.concatenate([here[k] for k in odd], axis=0)
    parts_odd = gathered(joined)
    hidden_even, near_even, far_even = expert_rows(even, parts_even, False)
    hidden_odd, near_odd, far_odd = expert_rows(odd, after(parts_odd, hidden_even), True)
    gathered_even = gathered(hidden_even)
    sums_even = expert_sums(even, after(gathered_even, hidden_odd), near_even, far_even)
    gathered_odd = [hidden_odd] + [across(hidden_odd, j) for j in range(1, T)]
    sums_odd = expert_sums(odd, after(gathered_odd, sums_even), near_odd, far_odd)
    routed = sums_even[0]
    for sums, group in ((sums_even, even), (sums_odd, odd)):
        for i, k in enumerate(group):
            if k > 0:
                routed = routed + zshift(sums[i].astype(BF), -k).astype(F32)
    return (stream + routed).astype(BF)


def solution(mesh):
    placed = (
        P("sp", "tp"),
        P("sp", "tp"),
        P("sp", "tp"),
        P("sp", "tp"),
        P("sp", "tp"),
        P("sp", None, "tp"),
        P("sp", None, "tp"),
        P("sp", None, "tp"),
        P(None, "tp"),
        P(None, "sp", "tp"),
        P("tp"),
        P("sp", None),
        P("sp", None),
        P("sp", None, "tp"),
        P("sp", None, "tp"),
        P("sp", None, "tp"),
    )

    return jax.shard_map(
        per_device, mesh=mesh, in_specs=placed, out_specs=P("sp", "tp"), check_vma=False
    )
```
